32 devices in a mesh: kv: 8 (over z, y), tp: 4 (over x, core).
Axes of the slice: x: 2, y: 2, z: 4, core: 2. Of those that a mesh axis runs over, the one named last changes fastest.
Arguments:
- tokens: bfloat16 [64, 2048], replicated, may hold values from -60 to 60
- mix_gain: float32 [2048], replicated, may hold values from 0.1 to 1.9
- query_weight: bfloat16 [2048, 1024], P(None, 'tp'), may hold values from -0.125 to 0.125
- key_weight: bfloat16 [2048, 1024], P(None, 'tp'), may hold values from -0.125 to 0.125
- value_weight: bfloat16 [2048, 1024], P(None, 'tp'), may hold values from -0.125 to 0.125
- gate_weight: bfloat16 [2048, 16], replicated, may hold values from -0.125 to 0.125
- gate_bias: float32 [16], replicated, may hold values from -1 to 3
- query_gain: float32 [64], replicated, may hold values from 0.1 to 1.9
- key_gain: float32 [64], replicated, may hold values from 0.1 to 1.9
- cache_keys: bfloat16 [4, 4096, 1024], P(None, 'kv', 'tp'), may hold values from -6 to 6
- cache_values: bfloat16 [4, 4096, 1024], P(None, 'kv', 'tp'), may hold values from -6 to 6
- cached_gates: float32 [4, 16, 4096], P(None, 'tp', 'kv'), as said below
- filled: int32 [4], replicated, may hold values from 1024 to 4063
- accepted: int32 [4], replicated, may hold values from 0 to 16
- parents: int32 [4, 16], replicated, may hold values from -1 to 14, as said below
- out_weight: bfloat16 [1024, 2048], P('tp', 'kv'), may hold values from -0.1875 to 0.1875
Outputs:
- mixed: bfloat16 [64, 2048], P('tp', 'kv')
- new_keys: bfloat16 [4, 4096, 1024], P(None, 'kv', 'tp')
- new_values: bfloat16 [4, 4096, 1024], P(None, 'kv', 'tp')
- new_gates: float32 [4, 16, 4096], P(None, 'tp', 'kv')
The draws below stay inside these ranges and needn't reach their ends.
Inputs may be any that keep to these rules, and one draw needn't show every extreme that they name: cached_gates[b, h, p] never rises as p grows. parents[b, 0] is -1 and, for t of 1 or more, parents[b, t] lies in 0 to t - 1, so a sequence's proposals form a tree.
All inputs are finite; a program needn't handle non-finite values.
Results may differ from the reference program's by a relative error of at most 0.013.
Values may be sent and summed in bfloat16 or wider, within the bound.
A program may use at most 64 MiB of HBM per device.

```python
import math
import jax
import jax.numpy as jnp
from jax import lax

D = 2048
ATTENDER_TOTAL = 16
HEAD_DIM = 64
PROPOSALS = 16
POS_DEV = 512
BATCH_ROWS = 4
MEMORY_SLOTS = 4096
N_TP = 4


def draw_tokens(key, part):
    derived_seeds = jax.random.split(jax.random.fold_in(key, 11), 2)
    columns = jnp.arange(D, dtype=jnp.float32)
    column_scale = jnp.exp(math.log(10.0) * columns / D) * jax.random.uniform(derived_seeds[1], (D,), jnp.float32, 0.5, 1.0)
    samples = jax.random.normal(derived_seeds[0], (BATCH_ROWS * PROPOSALS, D), jnp.float32)
    return jnp.clip(samples * column_scale, -60.0, 60.0).astype(jnp.bfloat16)


def draw_cached_gates(key, part):
    derived_seeds = jax.random.split(jax.random.fold_in(key, 23), 7)
    slow_share = 0.5
    slow_heads = jax.random.uniform(derived_seeds[0], (BATCH_ROWS, ATTENDER_TOTAL, 1), jnp.float32) < slow_share
    slow_rate = jnp.exp(jax.random.uniform(derived_seeds[1], (BATCH_ROWS, ATTENDER_TOTAL, 1), jnp.float32, math.log(0.3), math.log(1.5))) / MEMORY_SLOTS
    fast_rate = 1.0 / jax.random.uniform(derived_seeds[2], (BATCH_ROWS, ATTENDER_TOTAL, 1), jnp.float32, 30.0, 100.0)
    decay_rate = jnp.where(slow_heads, slow_rate, fast_rate)
    block_factor = jnp.exp(jax.random.uniform(derived_seeds[3], (BATCH_ROWS, ATTENDER_TOTAL, MEMORY_SLOTS // POS_DEV), jnp.float32, math.log(0.5), math.log(2.0)))
    block_factor = jnp.repeat(block_factor, POS_DEV, axis=2)
    roughness = jnp.exp(jax.random.uniform(derived_seeds[4], (BATCH_ROWS, ATTENDER_TOTAL, MEMORY_SLOTS), jnp.float32, -0.7, 0.7))
    jump_span = -decay_rate * block_factor * roughness
    spike_bundles = jax.random.uniform(derived_seeds[5], (BATCH_ROWS, ATTENDER_TOTAL, MEMORY_SLOTS), jnp.float32) < 3.0 / MEMORY_SLOTS
    dropped_amount = jnp.log(jax.random.uniform(derived_seeds[6], (BATCH_ROWS, ATTENDER_TOTAL, MEMORY_SLOTS), jnp.float32, 0.5, 0.8))
    jump_span = jump_span + jnp.where(spike_bundles, dropped_amount, 0.0)
    return jnp.cumsum(jump_span, axis=2).astype(jnp.float32)


def draw_parents(key, part):
    labels = jnp.arange(PROPOSALS, dtype=jnp.int32)
    limits = jnp.broadcast_to(jnp.maximum(labels, 1)[None, :], (BATCH_ROWS, PROPOSALS))
    chosen_parents = jax.random.randint(jax.random.fold_in(key, 37), (BATCH_ROWS, PROPOSALS), 0, limits, dtype=jnp.int32)
    return jnp.where(labels[None, :] == 0, -1, chosen_parents).astype(jnp.int32)


def with_ends(drawn, rng, low, largest):
    place = [jax.random.randint(jax.random.fold_in(rng, axis), (), 0, length) for axis, length in enumerate(drawn.shape)]
    widest = drawn.shape.index(max(drawn.shape))
    next_to = place[:widest] + [(place[widest] + 1) % drawn.shape[widest]] + place[widest + 1:]
    return drawn.at[tuple(place)].set(low).at[tuple(next_to)].set(largest)


def shard_levels(own_key, dims, shards, least, top_value):
    def one(dim, parts):
        draws = jax.random.uniform(jax.random.fold_in(jax.random.fold_in(own_key, 6), dim), (parts,), jnp.float32, least / len(shards), top_value / len(shards))
        return jnp.repeat(jnp.exp(draws), dims[dim] // parts).reshape((-1,) + (1,) * (len(dims) - dim - 1))

    loudness = one(*shards[0])
    for cut in shards[1:]:
        loudness = loudness * one(*cut)
    return loudness


def gaussian(rng, dims, deviation, limit, cuts=(), kind=jnp.bfloat16):
    gain = shard_levels(rng, dims, cuts, -0.22, 0.18) if cuts else 1.0
    drawn = jax.random.normal(rng, dims, jnp.float32) * deviation * gain
    return jnp.minimum(jnp.maximum(drawn, -limit), limit).astype(kind)


def setup_inputs(seed: int = 0) -> dict:
    keys = jax.random.split(jax.random.key(seed), 17)
    return {
        "tokens": draw_tokens(jax.random.fold_in(keys[16], 71), 0),
        "mix_gain": jnp.clip(1.0 + 0.18 * jax.random.normal(keys[1], (D,), jnp.float32), 0.1, 1.9),
        "query_weight": gaussian(keys[2], (D, ATTENDER_TOTAL * HEAD_DIM), D ** -0.5, 0.125, ((1, 4),)),
        "key_weight": gaussian(keys[3], (D, ATTENDER_TOTAL * HEAD_DIM), D ** -0.5, 0.125, ((1, 4),)),
        "value_weight": gaussian(keys[4], (D, ATTENDER_TOTAL * HEAD_DIM), D ** -0.5, 0.125, ((1, 4),)),
        "gate_weight": gaussian(keys[5], (D, ATTENDER_TOTAL), D ** -0.5, 0.125),
        "gate_bias": jnp.clip(jax.random.uniform(keys[6], (ATTENDER_TOTAL,), jnp.float32, -1.0, 3.0), -1.0, 3.0),
        "query_gain": jnp.clip(1.0 + 0.18 * jax.random.normal(keys[7], (HEAD_DIM,), jnp.float32), 0.1, 1.9),
        "key_gain": jnp.clip(1.0 + 0.18 * jax.random.normal(keys[8], (HEAD_DIM,), jnp.float32), 0.1, 1.9),
        "cache_keys": gaussian(keys[9], (BATCH_ROWS, MEMORY_SLOTS, ATTENDER_TOTAL * HEAD_DIM), 1.0, 6.0, ((1, 8), (2, 4))),
        "cache_values": gaussian(keys[10], (BATCH_ROWS, MEMORY_SLOTS, ATTENDER_TOTAL * HEAD_DIM), 1.0, 6.0, ((1, 8), (2, 4))),
        "cached_gates": draw_cached_gates(jax.random.fold_in(keys[16], 71), 0),
        "filled": with_ends(jax.random.randint(keys[12], (BATCH_ROWS,), MEMORY_SLOTS // 4, MEMORY_SLOTS - 2 * PROPOSALS), jax.random.fold_in(keys[12], 1), MEMORY_SLOTS // 4, (MEMORY_SLOTS - 2 * PROPOSALS) - 1).astype(jnp.int32),
        "accepted": with_ends(jax.random.randint(keys[13], (BATCH_ROWS,), 0, PROPOSALS + 1), jax.random.fold_in(keys[13], 1), 0, PROPOSALS).astype(jnp.int32),
        "parents": draw_parents(jax.random.fold_in(keys[16], 71), 0),
        "out_weight": gaussian(keys[15], (ATTENDER_TOTAL * HEAD_DIM, D), (ATTENDER_TOTAL * HEAD_DIM) ** -0.5, 0.1875, ((0, 4), (1, 8))),
    }


epsilon = 1e-06

def ancestry(parents):
    length = parents.shape[1]
    labels = jnp.arange(length, dtype=jnp.int32)
    start_nodes = jnp.broadcast_to(labels[None, :], parents.shape).astype(jnp.int32)
    start_running = (start_nodes[:, :, None] == labels[None, None, :]).astype(jnp.float32)

    def climb_once(step, carry):
        nodes, running = carry
        lifted = jnp.take_along_axis(parents, jnp.maximum(nodes, 0), axis=1).astype(jnp.int32)
        nodes = jnp.where(nodes >= 0, lifted, -1).astype(jnp.int32)
        running = running + (nodes[:, :, None] == labels[None, None, :]).astype(jnp.float32)
        return (nodes, running)
    finished = lax.fori_loop(0, length - 1, climb_once, (start_nodes, start_running))
    return finished[1]

def climb_sum(ancestors, log_gates):
    return lax.optimization_barrier(jnp.sum(ancestors[:, :, :, None] * log_gates[:, None, :, :], axis=2))

def head_norm(values, head_gain):
    return (values * lax.rsqrt(lax.optimization_barrier(jnp.mean(values * values, axis=-1, keepdims=True)) + epsilon) * head_gain).astype(jnp.bfloat16)

def write_keys(previous, incoming, offset):
    return lax.dynamic_update_slice(previous, incoming, (offset, jnp.int32(0)))

def write_gates(previous, incoming, offset):
    return lax.dynamic_update_slice(previous, incoming, (jnp.int32(0), offset))

def reference(tokens, mix_gain, query_weight, key_weight, value_weight, gate_weight, gate_bias, query_gain, key_gain, cache_keys, cache_values, cached_gates, filled, accepted, parents, out_weight):
    all_width = ATTENDER_TOTAL * HEAD_DIM
    floats = tokens.astype(jnp.float32)
    row_scale = lax.rsqrt(lax.optimization_barrier(jnp.mean(floats * floats, axis=1, keepdims=True)) + epsilon)
    scaled = (floats * mix_gain).astype(jnp.bfloat16)

    def project(weight):
        return jnp.dot(scaled, weight, preferred_element_type=jnp.float32) * row_scale
    queries = head_norm(project(query_weight).reshape(BATCH_ROWS, PROPOSALS, ATTENDER_TOTAL, HEAD_DIM), query_gain)
    fresh_keys = head_norm(project(key_weight).reshape(BATCH_ROWS, PROPOSALS, ATTENDER_TOTAL, HEAD_DIM), key_gain)
    fresh_values = project(value_weight).astype(jnp.bfloat16).reshape(BATCH_ROWS, PROPOSALS, ATTENDER_TOTAL, HEAD_DIM)
    log_gates = jax.nn.log_sigmoid(project(gate_weight) + gate_bias).reshape(BATCH_ROWS, PROPOSALS, ATTENDER_TOTAL)
    counts = filled + accepted
    picker = jnp.broadcast_to((counts - 1)[:, None, None], (BATCH_ROWS, ATTENDER_TOTAL, 1)).astype(jnp.int32)
    last_gate = jnp.take_along_axis(cached_gates, picker, axis=2)[:, :, 0]
    ancestors = ancestry(parents)
    climbed = climb_sum(ancestors, log_gates)
    fresh_gates = last_gate[:, None, :] + climbed
    factor = HEAD_DIM ** (-0.5)
    positions = jnp.arange(MEMORY_SLOTS, dtype=jnp.int32)

    def attend(inputs):
        query, key_new, value_new, past_keys, past_values, past_gates, climbing, gate_rows, tree_rows, live_count = inputs
        query_float = query.astype(jnp.float32)
        scores = jnp.einsum('thd,phd->htp', query_float, past_keys.reshape(MEMORY_SLOTS, ATTENDER_TOTAL, HEAD_DIM).astype(jnp.float32)) * factor
        scores = scores + jnp.transpose(gate_rows)[:, :, None] - past_gates[:, None, :]
        weights = jnp.where((positions < live_count)[None, None, :], jnp.exp(scores), 0.0)
        climb_heads = jnp.transpose(climbing)
        tree_scores = jnp.einsum('thd,uhd->htu', query_float, key_new.astype(jnp.float32)) * factor
        tree_scores = tree_scores + climb_heads[:, :, None] - climb_heads[:, None, :]
        tree_weights = jnp.where(tree_rows[None] > 0.5, jnp.exp(tree_scores), 0.0)
        denominator = lax.optimization_barrier(jnp.sum(weights, axis=2)) + lax.optimization_barrier(jnp.sum(tree_weights, axis=2))
        rounded = lax.optimization_barrier(weights.astype(jnp.bfloat16)).astype(jnp.float32)
        tree_rounded = lax.optimization_barrier(tree_weights.astype(jnp.bfloat16)).astype(jnp.float32)
        numerator = jnp.einsum('htp,phd->thd', rounded, past_values.reshape(MEMORY_SLOTS, ATTENDER_TOTAL, HEAD_DIM).astype(jnp.float32))
        numerator = numerator + jnp.einsum('htu,uhd->thd', tree_rounded, value_new.astype(jnp.float32))
        return (numerator / jnp.transpose(denominator)[:, :, None]).astype(jnp.bfloat16).reshape(PROPOSALS, all_width)
    attended = lax.map(attend, (queries, fresh_keys, fresh_values, cache_keys, cache_values, cached_gates, climbed, fresh_gates, ancestors, counts))
    attended = attended.reshape(BATCH_ROWS * PROPOSALS, all_width)
    group_width = all_width // N_TP
    mixed = jnp.zeros((BATCH_ROWS * PROPOSALS, D), jnp.float32)
    for member in range(N_TP):
        term = jnp.dot(attended[:, member * group_width:(member + 1) * group_width], out_weight[member * group_width:(member + 1) * group_width], preferred_element_type=jnp.float32).astype(jnp.bfloat16)
        mixed = mixed + lax.optimization_barrier(term).astype(jnp.float32)
    mixed = mixed.astype(jnp.bfloat16)
    new_keys = jax.vmap(write_keys)(cache_keys, fresh_keys.reshape(BATCH_ROWS, PROPOSALS, all_width), counts)
    new_values = jax.vmap(write_keys)(cache_values, fresh_values.reshape(BATCH_ROWS, PROPOSALS, all_width), counts)
    new_gates = jax.vmap(write_gates)(cached_gates, jnp.transpose(fresh_gates, (0, 2, 1)), counts)
    return (mixed, new_keys, new_values, new_gates)
```

```python
from functools import partial

import jax
import jax.numpy as jnp
from jax import lax
from jax.experimental import pallas as pl
from jax.experimental.pallas import tpu as pltpu
from jax.sharding import PartitionSpec as P

epsilon = 1e-06
SHIFT = 16.0
FAR = float(2.0**100)
LANES = 128
F32 = jnp.float32
BF16 = jnp.bfloat16
HIGH = lax.Precision.HIGHEST
VMEM = pltpu.VMEM


def iota(shape, axis):
    return lax.broadcasted_iota(jnp.int32, shape, axis)


def head_kernel(
    tokens, mix_gain, gate_weight, gate_bias, query_gain, key_gain, gates, parents,
    filled, accepted, wq, wk, wv, cache_keys, cache_values,
    message, tree, base, mask, new_keys, new_values,
    wbuf, kbuf, vbuf, wsem, ksem, vsem, osem,
):
    kv_rank = lax.axis_index("kv")
    tp_rank = lax.axis_index("tp")
    seqs, length, width = kbuf.shape
    heads = gates.shape[1]
    size = width // heads
    props = parents.shape[1]
    rows = seqs * props
    loads = []
    for i, w in enumerate((wq, wk)):
        loads.append(pltpu.make_async_copy(w, wbuf.at[i], wsem.at[i]))
    key_in = [pltpu.make_async_copy(cache_keys.at[b], kbuf.at[b], ksem.at[b]) for b in range(seqs)]
    value_in = [
        pltpu.make_async_copy(cache_values.at[b], vbuf.at[b], vsem.at[b]) for b in range(seqs)
    ]
    loads.append(pltpu.make_async_copy(wv, wbuf.at[2], wsem.at[2]))
    for c in loads[:2] + key_in + loads[2:] + value_in:
        c.start()

    floats = tokens[...].astype(F32)
    row_scale = lax.rsqrt(jnp.mean(floats * floats, axis=1, keepdims=True) + epsilon)
    scaled = (floats * mix_gain[...]).astype(BF16)

    parent_row = jnp.concatenate([parents[b : b + 1, :] for b in range(seqs)], axis=1)
    up = iota((rows, rows), 0)
    across = iota((rows, rows), 1)
    same = (up // props) == (across // props)
    power = (
        jnp.logical_and(same, jnp.broadcast_to(parent_row, (rows, rows)) == up % props)
        .astype(F32)
        .astype(BF16)
    )
    anc = (up == across).astype(F32) + power.astype(F32)
    reach = 2
    while reach < props:
        power = jnp.dot(power, power, preferred_element_type=F32).astype(BF16)
        anc = anc + jnp.dot(anc.astype(BF16), power, preferred_element_type=F32)
        reach *= 2
    ancestors = jnp.transpose(anc)

    gate_pre = jnp.dot(scaled, gate_weight[...], preferred_element_type=F32) * row_scale
    gate_pre = gate_pre + gate_bias[...]
    log_gates = jnp.minimum(gate_pre, 0.0) - jnp.log1p(jnp.exp(-jnp.abs(gate_pre)))
    all_heads = log_gates.shape[1]
    pick = iota((all_heads, LANES), 0) == tp_rank * heads + iota((all_heads, LANES), 1)
    pick = jnp.logical_and(pick, iota((all_heads, LANES), 1) < heads).astype(F32)
    local_gates = jnp.dot(log_gates, pick, preferred_element_type=F32, precision=HIGH)
    climb = jnp.dot(ancestors, local_gates, preferred_element_type=F32, precision=HIGH)
    climb_across = jnp.transpose(climb)

    def normed(full, gain):
        parts = []
        for h in range(heads):
            part = full[:, h * size : (h + 1) * size]
            scale = lax.rsqrt(jnp.mean(part * part, axis=1, keepdims=True) + epsilon)
            parts.append(part * scale * gain)
        return parts

    def project(i):
        loads[i].wait()
        return jnp.dot(scaled, wbuf[i], preferred_element_type=F32) * row_scale

    factor = size ** (-0.5)
    query = [
        (q.astype(BF16).astype(F32) * factor).astype(BF16)
        for q in normed(project(0), query_gain[...])
    ]
    fresh_key_heads = [k.astype(BF16) for k in normed(project(1), key_gain[...])]
    query_all = jnp.concatenate(query, axis=1)
    fresh_keys = jnp.concatenate(fresh_key_heads, axis=1)
    fresh_values = project(2).astype(BF16)

    window = 2 * props
    lane_head = iota((props, width), 1) // size
    block_head = iota((heads * props, width), 1) // size
    block_row = iota((heads * props, width), 0) // props
    diagonal = block_head == block_row
    positions = kv_rank * length + iota((heads, length), 1)
    lane = iota((props, LANES), 1)
    out_copies = []
    refs = []
    for b in range(seqs):
        count = filled[b] + accepted[b]
        live = positions < count
        own = gates[b]
        refs.append(jnp.min(jnp.where(live, own, FAR), axis=1, keepdims=True))
    for b in range(seqs):
        lo = b * props
        count = filled[b] + accepted[b]
        live = positions < count
        own = gates[b]
        ref = refs[b]
        shifted = jnp.where(live, ref - own - SHIFT, -FAR)
        spread = jnp.concatenate(
            [jnp.broadcast_to(shifted[h : h + 1, :], (props, length)) for h in range(heads)], axis=0
        )
        climb_col = jnp.concatenate([climb[lo : lo + props, h : h + 1] for h in range(heads)], axis=0)
        tiled = jnp.concatenate([query_all[lo : lo + props, :]] * heads, axis=0)
        tiled = jnp.where(diagonal, tiled, jnp.zeros_like(tiled))
        key_in[b].wait()
        scores = lax.dot_general(
            tiled, kbuf[b], (((1,), (1,)), ((), ())), preferred_element_type=F32
        )
        weights = jnp.exp(scores + climb_col + spread)
        den = jnp.sum(weights, axis=1, keepdims=True)
        value_in[b].wait()
        full = jnp.dot(weights.astype(BF16), vbuf[b], preferred_element_type=F32)
        num = jnp.zeros((props, width), F32)
        side = jnp.zeros((props, LANES), F32)
        for h in range(heads):
            num = jnp.where(lane_head == h, full[h * props : (h + 1) * props, :], num)
            side = jnp.where(lane == h, den[h * props : (h + 1) * props, :], side)
            side = jnp.where(lane == heads + h, ref[h : h + 1, :], side)
            for other in range(seqs):
                side = jnp.where(
                    lane == (2 + other) * heads + h, refs[other][h : h + 1, :], side
                )
        message[lo : lo + props, :width] = num
        message[lo : lo + props, width:] = side

        offset = count - kv_rank * length
        start = jnp.clip((offset // props) * props, 0, length - window)
        start = pl.multiple_of(start, props)
        rel = start + iota((window, props), 0) - offset
        one_hot = (rel == iota((window, props), 1)).astype(F32).astype(BF16)
        row_rel = start + iota((window, width), 0) - offset
        inside = jnp.logical_and(row_rel >= 0, row_rel < props)
        for fresh, buf, out, i in (
            (fresh_keys, kbuf, new_keys, 0),
            (fresh_values, vbuf, new_values, 1),
        ):
            placed = jnp.dot(one_hot, fresh[lo : lo + props, :], preferred_element_type=F32)
            old = buf[b, pl.ds(start, window), :].astype(F32)
            buf[b, pl.ds(start, window), :] = jnp.where(inside, placed, old).astype(BF16)
            c = pltpu.make_async_copy(buf.at[b], out.at[b], osem.at[i, b])
            c.start()
            out_copies.append(c)

        gate_rel = positions - count
        chosen = jnp.logical_and(gate_rel >= 0, gate_rel < props)
        placed_gates = own
        for t in range(props):
            column = jnp.concatenate(
                [climb[lo + t : lo + t + 1, h : h + 1] for h in range(heads)], axis=0
            )
            placed_gates = jnp.where(gate_rel == t, column, placed_gates)
        base[b] = placed_gates
        mask[b] = chosen.astype(F32)

    tree_side = jnp.zeros((rows, LANES), F32)
    row_lane = iota((rows, LANES), 1)
    tree_parts = []
    for h in range(heads):
        scores = lax.dot_general(
            query[h], fresh_key_heads[h], (((1,), (1,)), ((), ())), preferred_element_type=F32
        )
        scores = scores + climb[:, h : h + 1] - climb_across[h : h + 1, :] - SHIFT
        weights = jnp.exp(jnp.where(ancestors > 0.5, scores, -FAR))
        tree_side = jnp.where(row_lane == h, jnp.sum(weights, axis=1, keepdims=True), tree_side)
        tree_parts.append(
            jnp.dot(
                weights.astype(BF16),
                fresh_values[:, h * size : (h + 1) * size],
                preferred_element_type=F32,
            )
        )
    tree[:, :width] = jnp.concatenate(tree_parts, axis=1)
    tree[:, width:] = tree_side
    for c in out_copies:
        c.wait()


def tail_kernel(
    kv_size, tp_size, heads, message, tree, base, mask, weight,
    mixed, new_gates,
    inbox, attended, rows_in, weights_in, send1, recv1, send2, recv2, send3, recv3,
):
    k = lax.axis_index("kv")
    j = lax.axis_index("tp")
    total = kv_size * tp_size
    me = k * tp_size + j
    piece = message.shape[1]
    width = attended.shape[1]
    size = width // heads
    seqs = base.shape[0]
    slots = rows_in.shape[0]
    per_owner = slots // tp_size
    owner = k // per_owner
    barrier = pltpu.get_barrier_semaphore()

    def greet(s, carry):
        other = lax.rem(me + s, total)
        pl.semaphore_signal(
            barrier, inc=1, device_id={"kv": other // tp_size, "tp": lax.rem(other, tp_size)}
        )
        return carry

    lax.fori_loop(1, total, greet, 0)
    pl.semaphore_wait(barrier, total - 1)

    first = []
    for s in range(1, kv_size):
        dst = lax.rem(k + s, kv_size)
        c = pltpu.make_async_remote_copy(
            src_ref=message.at[dst], dst_ref=inbox.at[k], send_sem=send1.at[s],
            recv_sem=recv1.at[k], device_id={"kv": dst},
        )
        c.start()
        first.append(c)
    third = []
    for s in range(1, tp_size):
        dst = lax.rem(j + s, tp_size)
        c = pltpu.make_async_remote_copy(
            src_ref=weight, dst_ref=weights_in.at[j], send_sem=send3.at[s],
            recv_sem=recv3.at[j], device_id={"tp": dst},
        )
        c.start()
        third.append(c)
    inbox[k] = message[k]
    weights_in[j] = weight[...]
    for s in range(1, kv_size):
        src = lax.rem(k + kv_size - s, kv_size)
        pltpu.make_async_remote_copy(
            src_ref=message.at[src], dst_ref=inbox.at[src], send_sem=send1.at[s],
            recv_sem=recv1.at[src], device_id={"kv": src},
        ).wait_recv()

    last = inbox[0][:, width + heads : width + 2 * heads]
    for i in range(1, kv_size):
        last = jnp.minimum(last, inbox[i][:, width + heads : width + 2 * heads])
    scales = []
    own_tree = tree[k]
    den = own_tree[:, width : width + heads]
    for i in range(kv_size):
        scale = jnp.exp(last - inbox[i][:, width + heads : width + 2 * heads])
        den = den + scale * inbox[i][:, width : width + heads]
        scales.append(scale)

    def spread(x):
        return jnp.concatenate(
            [jnp.broadcast_to(x[:, h : h + 1], (piece, size)) for h in range(heads)], axis=1
        )

    num = own_tree[:, :width]
    for i in range(kv_size):
        num = num + spread(scales[i]) * inbox[i][:, :width]
    result = (num / spread(den)).astype(BF16).astype(F32)
    attended[...] = result

    slot = j * per_owner + lax.rem(k, per_owner)
    second = []
    for s in range(kv_size):
        dst = lax.rem(k + s, kv_size)
        second.append(
            pltpu.make_async_remote_copy(
                src_ref=attended, dst_ref=rows_in.at[slot], send_sem=send2.at[s],
                recv_sem=recv2.at[slot], device_id={"kv": dst, "tp": owner},
            )
        )
    for c in second[1:]:
        c.start()

    @pl.when(owner != j)
    def _():
        second[0].start()

    @pl.when(owner == j)
    def _():
        rows_in[slot] = result

    final = inbox[0][0:1, width:]
    for i in range(1, kv_size):
        final = jnp.minimum(final, inbox[i][0:1, width:])
    for b in range(seqs):
        at = (2 + b) * heads
        column = jnp.concatenate([final[:, at + h : at + h + 1] for h in range(heads)], axis=0)
        new_gates[b] = jnp.where(mask[b] > 0.5, base[b] + column, base[b])

    for s in range(1, tp_size):
        src = lax.rem(j + tp_size - s, tp_size)
        pltpu.make_async_remote_copy(
            src_ref=weight, dst_ref=weights_in.at[src], send_sem=send3.at[s],
            recv_sem=recv3.at[src], device_id={"tp": src},
        ).wait_recv()
    for i in range(slots):
        from_k = j * per_owner + i % per_owner
        from_j = i // per_owner

        @pl.when(jnp.logical_or(from_k != k, from_j != j))
        def _():
            pltpu.make_async_remote_copy(
                src_ref=attended, dst_ref=rows_in.at[i], send_sem=send2.at[0],
                recv_sem=recv2.at[i], device_id={"kv": from_k, "tp": from_j},
            ).wait_recv()

    out = None
    for g in range(tp_size):
        left = jnp.concatenate(
            [rows_in[g * per_owner + i] for i in range(per_owner)], axis=0
        ).astype(BF16)
        term = jnp.dot(left, weights_in[g], preferred_element_type=F32).astype(BF16).astype(F32)
        out = term if out is None else out + term
    mixed[...] = out.astype(BF16)
    for c in first + third + second[1:]:
        c.wait_send()

    @pl.when(owner != j)
    def _():
        second[0].wait_send()


def body(
    kv_size, tp_size,
    tokens, mix_gain, query_weight, key_weight, value_weight, gate_weight, gate_bias,
    query_gain, key_gain, cache_keys, cache_values, cached_gates, filled, accepted,
    parents, out_weight,
):
    row_count, model = tokens.shape
    seqs, length, width = cache_keys.shape
    heads = cached_gates.shape[1]
    props = parents.shape[1]
    vm = pl.BlockSpec(memory_space=VMEM)
    sm = pl.BlockSpec(memory_space=pltpu.SMEM)
    hbm = pl.BlockSpec(memory_space=pl.ANY)
    wide = width + LANES
    message, tree, base, mask, new_keys, new_values = pl.pallas_call(
        head_kernel,
        out_shape=(
            jax.ShapeDtypeStruct((row_count, wide), F32),
            jax.ShapeDtypeStruct((row_count, wide), F32),
            jax.ShapeDtypeStruct(cached_gates.shape, F32),
            jax.ShapeDtypeStruct(cached_gates.shape, F32),
            jax.ShapeDtypeStruct(cache_keys.shape, BF16),
            jax.ShapeDtypeStruct(cache_values.shape, BF16),
        ),
        in_specs=[vm] * 8 + [sm] * 2 + [hbm] * 5,
        out_specs=[vm] * 4 + [hbm] * 2,
        scratch_shapes=[
            VMEM((3, model, width), BF16),
            VMEM(cache_keys.shape, BF16),
            VMEM(cache_values.shape, BF16),
            pltpu.SemaphoreType.DMA((3,)),
            pltpu.SemaphoreType.DMA((seqs,)),
            pltpu.SemaphoreType.DMA((seqs,)),
            pltpu.SemaphoreType.DMA((2, seqs)),
        ],
        compiler_params=pltpu.CompilerParams(vmem_limit_bytes=24 * 2**20),
        cost_estimate=pl.CostEstimate(
            flops=500_000_000, bytes_accessed=8 * 2**20, transcendentals=0
        ),
        name="head",
    )(
        tokens, mix_gain.reshape(1, -1), gate_weight, gate_bias.reshape(1, -1),
        query_gain.reshape(1, -1), key_gain.reshape(1, -1), cached_gates, parents,
        filled, accepted, query_weight, key_weight, value_weight, cache_keys, cache_values,
    )
    piece = row_count // kv_size
    slots = tp_size * (row_count // tp_size // piece)
    dma = pltpu.SemaphoreType.DMA
    mixed, new_gates = pl.pallas_call(
        partial(tail_kernel, kv_size, tp_size, heads),
        out_shape=(
            jax.ShapeDtypeStruct((row_count // tp_size, out_weight.shape[1]), BF16),
            jax.ShapeDtypeStruct(cached_gates.shape, F32),
        ),
        in_specs=[vm] * 5,
        out_specs=[vm] * 2,
        scratch_shapes=[
            VMEM((kv_size, piece, wide), F32),
            VMEM((piece, width), F32),
            VMEM((slots, piece, width), F32),
            VMEM((tp_size,) + out_weight.shape, BF16),
            dma((kv_size,)), dma((kv_size,)), dma((kv_size,)), dma((slots,)),
            dma((tp_size,)), dma((tp_size,)),
        ],
        compiler_params=pltpu.CompilerParams(
            collective_id=0, has_side_effects=True, vmem_limit_bytes=16 * 2**20
        ),
        name="tail",
    )(
        message.reshape(kv_size, piece, wide), tree.reshape(kv_size, piece, wide), base, mask,
        out_weight,
    )
    return (mixed, new_keys, new_values, new_gates)


def solution(mesh):
    return jax.shard_map(
        partial(body, mesh.shape["kv"], mesh.shape["tp"]),
        mesh=mesh,
        in_specs=(
            P(), P(), P(None, "tp"), P(None, "tp"), P(None, "tp"), P(), P(), P(), P(),
            P(None, "kv", "tp"), P(None, "kv", "tp"), P(None, "tp", "kv"), P(), P(), P(),
            P("tp", "kv"),
        ),
        out_specs=(P("tp", "kv"), P(None, "kv", "tp"), P(None, "kv", "tp"), P(None, "tp", "kv")),
        check_vma=False,
    )
```

```python
from functools import partial

import jax
import jax.numpy as jnp
from jax import lax
from jax.experimental import pallas as pl
from jax.experimental.pallas import tpu as pltpu
from jax.sharding import PartitionSpec as P

epsilon = 1e-06
SHIFT = 16.0
FAR = float(2.0**100)
LANES = 128
PART = 32
F32 = jnp.float32
BF16 = jnp.bfloat16
HIGH = lax.Precision.HIGHEST
VMEM = pltpu.VMEM


def iota(shape, axis):
    return lax.broadcasted_iota(jnp.int32, shape, axis)


def head_kernel(
    tokens, mix_gain, gate_weight, gate_bias, query_gain, key_gain, gates, parents,
    filled, accepted, wq, wk, wv, cache_keys, cache_values,
    message, queries_out, keys_out, values_out, climb_out, across_out, ancestors_out,
    new_keys, new_values,
    wbuf, kbuf, vbuf, wsem, ksem, vsem, osem,
):
    kv_rank = lax.axis_index("kv")
    tp_rank = lax.axis_index("tp")
    seqs, length, width = kbuf.shape
    heads = gates.shape[1]
    size = width // heads
    props = parents.shape[1]
    rows = seqs * props
    piece = message.shape[1]
    loads = []
    for i, w in enumerate((wq, wk)):
        loads.append(pltpu.make_async_copy(w, wbuf.at[i], wsem.at[i]))
    key_in = [pltpu.make_async_copy(cache_keys.at[b], kbuf.at[b], ksem.at[b]) for b in range(seqs)]
    value_in = [
        pltpu.make_async_copy(cache_values.at[b], vbuf.at[b], vsem.at[b]) for b in range(seqs)
    ]
    loads.append(pltpu.make_async_copy(wv, wbuf.at[2], wsem.at[2]))
    for c in loads[:2] + key_in + loads[2:] + value_in:
        c.start()

    floats = tokens[...].astype(F32)
    row_scale = lax.rsqrt(jnp.mean(floats * floats, axis=1, keepdims=True) + epsilon)
    scaled = (floats * mix_gain[...]).astype(BF16)

    parent_row = jnp.concatenate([parents[b : b + 1, :] for b in range(seqs)], axis=1)
    up = iota((rows, rows), 0)
    across = iota((rows, rows), 1)
    same = (up // props) == (across // props)
    power = (
        jnp.logical_and(same, jnp.broadcast_to(parent_row, (rows, rows)) == up % props)
        .astype(F32)
        .astype(BF16)
    )
    anc = (up == across).astype(F32) + power.astype(F32)
    reach = 2
    while reach < props:
        power = jnp.dot(power, power, preferred_element_type=F32).astype(BF16)
        anc = anc + jnp.dot(anc.astype(BF16), power, preferred_element_type=F32)
        reach *= 2
    ancestors = jnp.transpose(anc)

    gate_pre = (
        lax.dot_general(
            scaled, gate_weight[...], (((1,), (1,)), ((), ())), preferred_element_type=F32
        )
        * row_scale
    )
    gate_pre = gate_pre + gate_bias[...]
    log_gates = jnp.minimum(gate_pre, 0.0) - jnp.log1p(jnp.exp(-jnp.abs(gate_pre)))
    all_heads = log_gates.shape[1]
    pick = iota((all_heads, LANES), 0) == tp_rank * heads + iota((all_heads, LANES), 1)
    pick = jnp.logical_and(pick, iota((all_heads, LANES), 1) < heads).astype(F32)
    local_gates = jnp.dot(log_gates, pick, preferred_element_type=F32, precision=HIGH)
    climb = jnp.dot(ancestors, local_gates, preferred_element_type=F32, precision=HIGH)
    climb_across = jnp.transpose(climb)

    def normed(full, gain):
        parts = []
        for h in range(heads):
            part = full[:, h * size : (h + 1) * size]
            scale = lax.rsqrt(jnp.mean(part * part, axis=1, keepdims=True) + epsilon)
            parts.append(part * scale * gain)
        return parts

    def project(i):
        loads[i].wait()
        return jnp.dot(scaled, wbuf[i], preferred_element_type=F32) * row_scale

    factor = size ** (-0.5)
    query = [
        (q.astype(BF16).astype(F32) * factor).astype(BF16)
        for q in normed(project(0), query_gain[...])
    ]
    fresh_key_heads = [k.astype(BF16) for k in normed(project(1), key_gain[...])]
    query_all = jnp.concatenate(query, axis=1)
    fresh_keys = jnp.concatenate(fresh_key_heads, axis=1)
    fresh_values = project(2).astype(BF16)

    window = 2 * props
    lane_head = iota((props, width), 1) // size
    block_head = iota((heads * props, width), 1) // size
    block_row = iota((heads * props, width), 0) // props
    diagonal = block_head == block_row
    positions = kv_rank * length + iota((heads, length), 1)
    lane = iota((props, LANES), 1) % PART
    out_copies = []
    refs = []
    for b in range(seqs):
        count = filled[b] + accepted[b]
        live = positions < count
        own = gates[b]
        refs.append(jnp.min(jnp.where(live, own, FAR), axis=1, keepdims=True))
    for b in range(seqs):
        lo = b * props
        count = filled[b] + accepted[b]
        live = positions < count
        own = gates[b]
        ref = refs[b]
        shifted = jnp.where(live, ref - own - SHIFT, -FAR)
        spread = jnp.concatenate(
            [jnp.broadcast_to(shifted[h : h + 1, :], (props, length)) for h in range(heads)], axis=0
        )
        climb_col = jnp.concatenate([climb[lo : lo + props, h : h + 1] for h in range(heads)], axis=0)
        tiled = jnp.concatenate([query_all[lo : lo + props, :]] * heads, axis=0)
        tiled = jnp.where(diagonal, tiled, jnp.zeros_like(tiled))
        key_in[b].wait()
        scores = lax.dot_general(
            tiled, kbuf[b], (((1,), (1,)), ((), ())), preferred_element_type=F32
        )
        weights = jnp.exp(scores + climb_col + spread)
        den = jnp.sum(weights, axis=1, keepdims=True)
        value_in[b].wait()
        full = jnp.dot(weights.astype(BF16), vbuf[b], preferred_element_type=F32)
        num = jnp.zeros((props, width), F32)
        side = jnp.zeros((props, LANES), F32)
        for h in range(heads):
            num = jnp.where(lane_head == h, full[h * props : (h + 1) * props, :], num)
            side = jnp.where(lane == h, den[h * props : (h + 1) * props, :], side)
            side = jnp.where(lane == heads + h, ref[h : h + 1, :], side)
            for other in range(seqs):
                side = jnp.where(
                    lane == (2 + other) * heads + h, refs[other][h : h + 1, :], side
                )
        high = side.astype(BF16).astype(F32)
        middle = (side - high).astype(BF16).astype(F32)
        low = side - high - middle
        part = iota((props, LANES), 1) // PART
        side = jnp.where(part == 0, high, jnp.where(part == 1, middle, low))
        packed = jnp.concatenate([num, side], axis=1)
        for r in range(0, props, piece):
            message[(lo + r) // piece] = packed[r : r + piece].astype(BF16)

        offset = count - kv_rank * length
        start = jnp.clip((offset // props) * props, 0, length - window)
        start = pl.multiple_of(start, props)
        rel = start + iota((window, props), 0) - offset
        one_hot = (rel == iota((window, props), 1)).astype(F32).astype(BF16)
        row_rel = start + iota((window, width), 0) - offset
        inside = jnp.logical_and(row_rel >= 0, row_rel < props)
        for fresh, buf, out, i in (
            (fresh_keys, kbuf, new_keys, 0),
            (fresh_values, vbuf, new_values, 1),
        ):
            placed = jnp.dot(one_hot, fresh[lo : lo + props, :], preferred_element_type=F32)
            old = buf[b, pl.ds(start, window), :].astype(F32)
            buf[b, pl.ds(start, window), :] = jnp.where(inside, placed, old).astype(BF16)
            c = pltpu.make_async_copy(buf.at[b], out.at[b], osem.at[i, b])
            c.start()
            out_copies.append(c)

    queries_out[...] = query_all
    keys_out[...] = fresh_keys
    values_out[...] = fresh_values
    climb_out[...] = climb
    across_out[...] = climb_across
    ancestors_out[...] = ancestors
    for c in out_copies:
        c.wait()


def tail_kernel(
    kv_size, tp_size, heads, message, queries, fresh_keys, fresh_values, climb, across,
    ancestors, gates, weight, filled, accepted,
    mixed, new_gates,
    tree, inbox, attended, rows_in, weights_in, send1, recv1, send2, recv2, send3, recv3,
):
    k = lax.axis_index("kv")
    j = lax.axis_index("tp")
    total = kv_size * tp_size
    me = k * tp_size + j
    piece = message.shape[1]
    width = attended.shape[1]
    size = width // heads
    seqs, _, length = gates.shape
    rows = queries.shape[0]
    props = rows // seqs
    slots = rows_in.shape[0]
    per_owner = slots // tp_size
    owner = k // per_owner
    barrier = pltpu.get_barrier_semaphore()

    def greet(s, carry):
        other = lax.rem(me + s, total)
        pl.semaphore_signal(
            barrier, inc=1, device_id={"kv": other // tp_size, "tp": lax.rem(other, tp_size)}
        )
        return carry

    lax.fori_loop(1, total, greet, 0)
    pl.semaphore_wait(barrier, total - 1)

    first = []
    for s in range(1, kv_size):
        dst = lax.rem(k + s, kv_size)
        c = pltpu.make_async_remote_copy(
            src_ref=message.at[dst], dst_ref=inbox.at[k], send_sem=send1.at[s],
            recv_sem=recv1.at[k], device_id={"kv": dst},
        )
        c.start()
        first.append(c)
    third = []
    for s in range(1, tp_size):
        dst = lax.rem(j + s, tp_size)
        c = pltpu.make_async_remote_copy(
            src_ref=weight, dst_ref=weights_in.at[j], send_sem=send3.at[s],
            recv_sem=recv3.at[j], device_id={"tp": dst},
        )
        c.start()
        third.append(c)
    inbox[k] = message[k]
    weights_in[j] = weight[...]
    side = jnp.zeros((rows, LANES), F32)
    row_lane = iota((rows, LANES), 1)
    tree_parts = []
    for h in range(heads):
        at = slice(h * size, (h + 1) * size)
        scores = lax.dot_general(
            queries[:, at], fresh_keys[:, at], (((1,), (1,)), ((), ())),
            preferred_element_type=F32,
        )
        scores = scores + climb[:, h : h + 1] - across[h : h + 1, :] - SHIFT
        weights = jnp.exp(jnp.where(ancestors[...] > 0.5, scores, -FAR))
        side = jnp.where(row_lane == h, jnp.sum(weights, axis=1, keepdims=True), side)
        tree_parts.append(
            jnp.dot(weights.astype(BF16), fresh_values[:, at], preferred_element_type=F32)
        )
    packed = jnp.concatenate(tree_parts + [side], axis=1)
    for i in range(kv_size):
        tree[i] = packed[i * piece : (i + 1) * piece]
    positions = k * length + iota((heads, length), 1)
    chosen = []
    placed = []
    for b in range(seqs):
        rel = positions - (filled[b] + accepted[b])
        chosen.append(jnp.logical_and(rel >= 0, rel < props))
        climbs = jnp.zeros((heads, length), F32)
        for t in range(props):
            u = b * props + t
            column = jnp.broadcast_to(across[:heads, u : u + 1], (heads, length))
            climbs = jnp.where(rel == t, column, climbs)
        placed.append(climbs)
    for s in range(1, kv_size):
        src = lax.rem(k + kv_size - s, kv_size)
        pltpu.make_async_remote_copy(
            src_ref=message.at[src], dst_ref=inbox.at[src], send_sem=send1.at[s],
            recv_sem=recv1.at[src], device_id={"kv": src},
        ).wait_recv()

    parts = []
    sides = []
    for i in range(kv_size):
        got = inbox[i].astype(F32)
        parts.append(got[:, :width])
        side = got[:, width:]
        sides.append(
            side[:, :PART] + side[:, PART : 2 * PART] + side[:, 2 * PART : 3 * PART]
        )
    final = sides[0]
    for side in sides[1:]:
        final = jnp.minimum(final, side)
    last = final[:, heads : 2 * heads]
    own_tree = tree[k]
    den = own_tree[:, width : width + heads]
    scales = []
    for side in sides:
        scale = jnp.exp(last - side[:, heads : 2 * heads])
        den = den + scale * side[:, :heads]
        scales.append(scale)

    def spread(x):
        return jnp.concatenate(
            [jnp.broadcast_to(x[:, h : h + 1], (piece, size)) for h in range(heads)], axis=1
        )

    num = own_tree[:, :width]
    for i in range(kv_size):
        num = num + spread(scales[i]) * parts[i]
    result = (num / spread(den)).astype(BF16)
    attended[...] = result

    slot = j * per_owner + lax.rem(k, per_owner)
    second = []
    for s in range(kv_size):
        dst = lax.rem(k + s, kv_size)
        second.append(
            pltpu.make_async_remote_copy(
                src_ref=attended, dst_ref=rows_in.at[slot], send_sem=send2.at[s],
                recv_sem=recv2.at[slot], device_id={"kv": dst, "tp": owner},
            )
        )
    for c in second[1:]:
        c.start()

    @pl.when(owner != j)
    def _():
        second[0].start()

    @pl.when(owner == j)
    def _():
        rows_in[slot] = result

    final = final[0:1, :]
    for b in range(seqs):
        at = (2 + b) * heads
        column = jnp.concatenate([final[:, at + h : at + h + 1] for h in range(heads)], axis=0)
        new_gates[b] = jnp.where(chosen[b], placed[b] + column, gates[b])

    for s in range(1, tp_size):
        src = lax.rem(j + tp_size - s, tp_size)
        pltpu.make_async_remote_copy(
            src_ref=weight, dst_ref=weights_in.at[src], send_sem=send3.at[s],
            recv_sem=recv3.at[src], device_id={"tp": src},
        ).wait_recv()
    for i in range(slots):
        from_k = j * per_owner + i % per_owner
        from_j = i // per_owner

        @pl.when(jnp.logical_or(from_k != k, from_j != j))
        def _():
            pltpu.make_async_remote_copy(
                src_ref=attended, dst_ref=rows_in.at[i], send_sem=send2.at[0],
                recv_sem=recv2.at[i], device_id={"kv": from_k, "tp": from_j},
            ).wait_recv()

    out = None
    for g in range(tp_size):
        left = jnp.concatenate(
            [rows_in[g * per_owner + i].astype(F32) for i in range(per_owner)], axis=0
        ).astype(BF16)
        term = jnp.dot(left, weights_in[g], preferred_element_type=F32).astype(BF16).astype(F32)
        out = term if out is None else out + term
    mixed[...] = out.astype(BF16)
    for c in first + third + second[1:]:
        c.wait_send()

    @pl.when(owner != j)
    def _():
        second[0].wait_send()


def body(
    kv_size, tp_size,
    tokens, mix_gain, query_weight, key_weight, value_weight, gate_weight, gate_bias,
    query_gain, key_gain, cache_keys, cache_values, cached_gates, filled, accepted,
    parents, out_weight,
):
    row_count, model = tokens.shape
    seqs, length, width = cache_keys.shape
    heads = cached_gates.shape[1]
    props = parents.shape[1]
    vm = pl.BlockSpec(memory_space=VMEM)
    sm = pl.BlockSpec(memory_space=pltpu.SMEM)
    hbm = pl.BlockSpec(memory_space=pl.ANY)
    wide = width + LANES
    piece = row_count // kv_size
    message, *carried, new_keys, new_values = pl.pallas_call(
        head_kernel,
        out_shape=(
            jax.ShapeDtypeStruct((kv_size, piece, wide), BF16),
            jax.ShapeDtypeStruct((row_count, width), BF16),
            jax.ShapeDtypeStruct((row_count, width), BF16),
            jax.ShapeDtypeStruct((row_count, width), BF16),
            jax.ShapeDtypeStruct((row_count, LANES), F32),
            jax.ShapeDtypeStruct((LANES, row_count), F32),
            jax.ShapeDtypeStruct((row_count, row_count), F32),
            jax.ShapeDtypeStruct(cache_keys.shape, BF16),
            jax.ShapeDtypeStruct(cache_values.shape, BF16),
        ),
        in_specs=[vm] * 8 + [sm] * 2 + [hbm] * 5,
        out_specs=[vm] * 7 + [hbm] * 2,
        scratch_shapes=[
            VMEM((3, model, width), BF16),
            VMEM(cache_keys.shape, BF16),
            VMEM(cache_values.shape, BF16),
            pltpu.SemaphoreType.DMA((3,)),
            pltpu.SemaphoreType.DMA((seqs,)),
            pltpu.SemaphoreType.DMA((seqs,)),
            pltpu.SemaphoreType.DMA((2, seqs)),
        ],
        compiler_params=pltpu.CompilerParams(vmem_limit_bytes=int(53.5 * 2**20)),
        cost_estimate=pl.CostEstimate(
            flops=500_000_000, bytes_accessed=8 * 2**20, transcendentals=0
        ),
        name="head",
    )(
        tokens, mix_gain.reshape(1, -1), jnp.transpose(gate_weight), gate_bias.reshape(1, -1),
        query_gain.reshape(1, -1), key_gain.reshape(1, -1), cached_gates, parents,
        filled, accepted, query_weight, key_weight, value_weight, cache_keys, cache_values,
    )
    slots = tp_size * (row_count // tp_size // piece)
    dma = pltpu.SemaphoreType.DMA
    mixed, new_gates = pl.pallas_call(
        partial(tail_kernel, kv_size, tp_size, heads),
        out_shape=(
            jax.ShapeDtypeStruct((row_count // tp_size, out_weight.shape[1]), BF16),
            jax.ShapeDtypeStruct(cached_gates.shape, F32),
        ),
        in_specs=[vm] * 9 + [sm] * 2,
        out_specs=[vm] * 2,
        scratch_shapes=[
            VMEM((kv_size, piece, wide), F32),
            VMEM((kv_size, piece, wide), BF16),
            VMEM((piece, width), BF16),
            VMEM((slots, piece, width), BF16),
            VMEM((tp_size,) + out_weight.shape, BF16),
            dma((kv_size,)), dma((kv_size,)), dma((kv_size,)), dma((slots,)),
            dma((tp_size,)), dma((tp_size,)),
        ],
        compiler_params=pltpu.CompilerParams(
            collective_id=0, has_side_effects=True, vmem_limit_bytes=16 * 2**20
        ),
        name="tail",
    )(
        message, *carried, cached_gates, out_weight, filled, accepted,
    )
    return (mixed, new_keys, new_values, new_gates)


def solution(mesh):
    return jax.shard_map(
        partial(body, mesh.shape["kv"], mesh.shape["tp"]),
        mesh=mesh,
        in_specs=(
            P(), P(), P(None, "tp"), P(None, "tp"), P(None, "tp"), P(), P(), P(), P(),
            P(None, "kv", "tp"), P(None, "kv", "tp"), P(None, "tp", "kv"), P(), P(), P(),
            P("tp", "kv"),
        ),
        out_specs=(P("tp", "kv"), P(None, "kv", "tp"), P(None, "kv", "tp"), P(None, "tp", "kv")),
        check_vma=False,
    )
```

```python
from functools import partial

import jax
import jax.numpy as jnp
from jax import lax
from jax.experimental import pallas as pl
from jax.experimental.pallas import tpu as pltpu
from jax.sharding import PartitionSpec as P

epsilon = 1e-06
SHIFT = 16.0
FAR = float(2.0**100)
LANES = 128
PART = 32
F32 = jnp.float32
BF16 = jnp.bfloat16
HIGH = lax.Precision.HIGHEST
VMEM = pltpu.VMEM


def iota(shape, axis):
    return lax.broadcasted_iota(jnp.int32, shape, axis)


def head_kernel(
    tokens, mix_gain, gate_weight, gate_bias, query_gain, key_gain, gates, parents,
    filled, accepted, wq, wk, wv, cache_keys, cache_values,
    message, queries_out, keys_out, values_out, climb_out, across_out, ancestors_out,
    new_keys, new_values,
    wbuf, kbuf, vbuf, wsem, ksem, vsem, osem,
):
    kv_rank = lax.axis_index("kv")
    tp_rank = lax.axis_index("tp")
    seqs, length, width = kbuf.shape
    heads = gates.shape[1]
    size = width // heads
    props = parents.shape[1]
    rows = seqs * props
    piece = message.shape[1]
    loads = []
    for i, w in enumerate((wq, wk)):
        loads.append(pltpu.make_async_copy(w, wbuf.at[i], wsem.at[i]))
    key_in = [pltpu.make_async_copy(cache_keys.at[b], kbuf.at[b], ksem.at[b]) for b in range(seqs)]
    value_in = [
        pltpu.make_async_copy(cache_values.at[b], vbuf.at[b], vsem.at[b]) for b in range(seqs)
    ]
    loads.append(pltpu.make_async_copy(wv, wbuf.at[2], wsem.at[2]))
    for c in loads[:2] + key_in + loads[2:] + value_in:
        c.start()

    floats = tokens[...].astype(F32)
    row_scale = lax.rsqrt(jnp.mean(floats * floats, axis=1, keepdims=True) + epsilon)
    scaled = (floats * mix_gain[...]).astype(BF16)

    parent_row = jnp.concatenate([parents[b : b + 1, :] for b in range(seqs)], axis=1)
    up = iota((rows, rows), 0)
    across = iota((rows, rows), 1)
    same = (up // props) == (across // props)
    power = (
        jnp.logical_and(same, jnp.broadcast_to(parent_row, (rows, rows)) == up % props)
        .astype(F32)
        .astype(BF16)
    )
    anc = (up == across).astype(F32) + power.astype(F32)
    reach = 2
    while reach < props:
        power = jnp.dot(power, power, preferred_element_type=F32).astype(BF16)
        anc = anc + jnp.dot(anc.astype(BF16), power, preferred_element_type=F32)
        reach *= 2
    ancestors = jnp.transpose(anc)

    gate_pre = (
        lax.dot_general(
            scaled, gate_weight[...], (((1,), (1,)), ((), ())), preferred_element_type=F32
        )
        * row_scale
    )
    gate_pre = gate_pre + gate_bias[...]
    log_gates = jnp.minimum(gate_pre, 0.0) - jnp.log1p(jnp.exp(-jnp.abs(gate_pre)))
    all_heads = log_gates.shape[1]
    pick = iota((all_heads, LANES), 0) == tp_rank * heads + iota((all_heads, LANES), 1)
    pick = jnp.logical_and(pick, iota((all_heads, LANES), 1) < heads).astype(F32)
    local_gates = jnp.dot(log_gates, pick, preferred_element_type=F32, precision=HIGH)
    climb = jnp.dot(ancestors, local_gates, preferred_element_type=F32, precision=HIGH)
    climb_across = jnp.transpose(climb)

    def normed(full, gain):
        parts = []
        for h in range(heads):
            part = full[:, h * size : (h + 1) * size]
            scale = lax.rsqrt(jnp.mean(part * part, axis=1, keepdims=True) + epsilon)
            parts.append(part * scale * gain)
        return parts

    def project(i):
        loads[i].wait()
        return jnp.dot(scaled, wbuf[i], preferred_element_type=F32) * row_scale

    factor = size ** (-0.5)
    query = [
        (q.astype(BF16).astype(F32) * factor).astype(BF16)
        for q in normed(project(0), query_gain[...])
    ]
    fresh_key_heads = [k.astype(BF16) for k in normed(project(1), key_gain[...])]
    query_all = jnp.concatenate(query, axis=1)
    fresh_keys = jnp.concatenate(fresh_key_heads, axis=1)
    fresh_values = project(2).astype(BF16)

    window = 2 * props
    lane_head = iota((props, width), 1) // size
    block_head = iota((heads * props, width), 1) // size
    block_row = iota((heads * props, width), 0) // props
    diagonal = block_head == block_row
    positions = kv_rank * length + iota((heads, length), 1)
    lane = iota((props, LANES), 1) % PART
    out_copies = []
    refs = []
    for b in range(seqs):
        count = filled[b] + accepted[b]
        live = positions < count
        own = gates[b]
        refs.append(jnp.min(jnp.where(live, own, FAR), axis=1, keepdims=True))
    for b in range(seqs):
        lo = b * props
        count = filled[b] + accepted[b]
        live = positions < count
        own = gates[b]
        ref = refs[b]
        shifted = jnp.where(live, ref - own - SHIFT, -FAR)
        spread = jnp.concatenate(
            [jnp.broadcast_to(shifted[h : h + 1, :], (props, length)) for h in range(heads)], axis=0
        )
        climb_col = jnp.concatenate([climb[lo : lo + props, h : h + 1] for h in range(heads)], axis=0)
        tiled = jnp.concatenate([query_all[lo : lo + props, :]] * heads, axis=0)
        tiled = jnp.where(diagonal, tiled, jnp.zeros_like(tiled))
        key_in[b].wait()
        scores = lax.dot_general(
            tiled, kbuf[b], (((1,), (1,)), ((), ())), preferred_element_type=F32
        )
        weights = jnp.exp(scores + climb_col + spread)
        den = jnp.sum(weights, axis=1, keepdims=True)
        value_in[b].wait()
        full = jnp.dot(weights.astype(BF16), vbuf[b], preferred_element_type=F32)
        num = jnp.zeros((props, width), F32)
        side = jnp.zeros((props, LANES), F32)
        for h in range(heads):
            num = jnp.where(lane_head == h, full[h * props : (h + 1) * props, :], num)
            side = jnp.where(lane == h, den[h * props : (h + 1) * props, :], side)
            side = jnp.where(lane == heads + h, ref[h : h + 1, :], side)
            for other in range(seqs):
                side = jnp.where(
                    lane == (2 + other) * heads + h, refs[other][h : h + 1, :], side
                )
        high = side.astype(BF16).astype(F32)
        middle = (side - high).astype(BF16).astype(F32)
        low = side - high - middle
        part = iota((props, LANES), 1) // PART
        side = jnp.where(part == 0, high, jnp.where(part == 1, middle, low))
        packed = jnp.concatenate([num, side], axis=1)
        for r in range(0, props, piece):
            message[(lo + r) // piece] = packed[r : r + piece].astype(BF16)

        offset = count - kv_rank * length
        start = jnp.clip((offset // props) * props, 0, length - window)
        start = pl.multiple_of(start, props)
        rel = start + iota((window, props), 0) - offset
        one_hot = (rel == iota((window, props), 1)).astype(F32).astype(BF16)
        row_rel = start + iota((window, width), 0) - offset
        inside = jnp.logical_and(row_rel >= 0, row_rel < props)
        for fresh, buf, out, i in (
            (fresh_keys, kbuf, new_keys, 0),
            (fresh_values, vbuf, new_values, 1),
        ):
            placed = jnp.dot(one_hot, fresh[lo : lo + props, :], preferred_element_type=F32)
            old = buf[b, pl.ds(start, window), :].astype(F32)
            buf[b, pl.ds(start, window), :] = jnp.where(inside, placed, old).astype(BF16)
            c = pltpu.make_async_copy(buf.at[b], out.at[b], osem.at[i, b])
            c.start()
            out_copies.append(c)

    queries_out[...] = query_all
    keys_out[...] = fresh_keys
    values_out[...] = fresh_values
    climb_out[...] = climb
    across_out[...] = climb_across
    ancestors_out[...] = ancestors
    for c in out_copies:
        c.wait()


def tail_kernel(
    kv_size, tp_size, heads, message, queries, fresh_keys, fresh_values, climb, across,
    ancestors, gates, weight, filled, accepted,
    mixed, new_gates,
    tree, inbox, attended, rows_in, weights_in, send1, recv1, send2, recv2, send3, recv3,
):
    k = lax.axis_index("kv")
    j = lax.axis_index("tp")
    total = kv_size * tp_size
    me = k * tp_size + j
    piece = message.shape[1]
    width = attended.shape[1]
    size = width // heads
    seqs, _, length = gates.shape
    rows = queries.shape[0]
    props = rows // seqs
    slots = rows_in.shape[0]
    per_owner = slots // tp_size
    owner = k // per_owner
    barrier = pltpu.get_barrier_semaphore()

    def greet(s, carry):
        other = lax.rem(me + s, total)
        pl.semaphore_signal(
            barrier, inc=1, device_id={"kv": other // tp_size, "tp": lax.rem(other, tp_size)}
        )
        return carry

    lax.fori_loop(1, total, greet, 0)
    pl.semaphore_wait(barrier, total - 1)

    first = []
    for s in range(1, kv_size):
        dst = lax.rem(k + s, kv_size)
        c = pltpu.make_async_remote_copy(
            src_ref=message.at[dst], dst_ref=inbox.at[k], send_sem=send1.at[s],
            recv_sem=recv1.at[k], device_id={"kv": dst},
        )
        c.start()
        first.append(c)
    third = []
    for s in range(1, tp_size):
        dst = lax.rem(j + s, tp_size)
        c = pltpu.make_async_remote_copy(
            src_ref=weight, dst_ref=weights_in.at[j], send_sem=send3.at[s],
            recv_sem=recv3.at[j], device_id={"tp": dst},
        )
        c.start()
        third.append(c)
    inbox[k] = message[k]
    weights_in[j] = weight[...]
    side = jnp.zeros((rows, LANES), F32)
    row_lane = iota((rows, LANES), 1)
    tree_parts = []
    for h in range(heads):
        at = slice(h * size, (h + 1) * size)
        scores = lax.dot_general(
            queries[:, at], fresh_keys[:, at], (((1,), (1,)), ((), ())),
            preferred_element_type=F32,
        )
        scores = scores + climb[:, h : h + 1] - across[h : h + 1, :] - SHIFT
        weights = jnp.exp(jnp.where(ancestors[...] > 0.5, scores, -FAR))
        side = jnp.where(row_lane == h, jnp.sum(weights, axis=1, keepdims=True), side)
        tree_parts.append(
            jnp.dot(weights.astype(BF16), fresh_values[:, at], preferred_element_type=F32)
        )
    packed = jnp.concatenate(tree_parts + [side], axis=1)
    for i in range(kv_size):
        tree[i] = packed[i * piece : (i + 1) * piece]
    positions = k * length + iota((heads, length), 1)
    chosen = []
    placed = []
    for b in range(seqs):
        rel = positions - (filled[b] + accepted[b])
        chosen.append(jnp.logical_and(rel >= 0, rel < props))
        climbs = jnp.zeros((heads, length), F32)
        for t in range(props):
            u = b * props + t
            column = jnp.broadcast_to(across[:heads, u : u + 1], (heads, length))
            climbs = jnp.where(rel == t, column, climbs)
        placed.append(climbs)
    for s in range(1, kv_size):
        src = lax.rem(k + kv_size - s, kv_size)
        pltpu.make_async_remote_copy(
            src_ref=message.at[src], dst_ref=inbox.at[src], send_sem=send1.at[s],
            recv_sem=recv1.at[src], device_id={"kv": src},
        ).wait_recv()

    parts = []
    sides = []
    for i in range(kv_size):
        got = inbox[i].astype(F32)
        parts.append(got[:, :width])
        side = got[:, width:]
        sides.append(
            side[:, :PART] + side[:, PART : 2 * PART] + side[:, 2 * PART : 3 * PART]
        )
    final = sides[0]
    for side in sides[1:]:
        final = jnp.minimum(final, side)
    last = final[:, heads : 2 * heads]
    own_tree = tree[k]
    den = own_tree[:, width : width + heads]
    scales = []
    for side in sides:
        scale = jnp.exp(last - side[:, heads : 2 * heads])
        den = den + scale * side[:, :heads]
        scales.append(scale)

    def spread(x):
        return jnp.concatenate(
            [jnp.broadcast_to(x[:, h : h + 1], (piece, size)) for h in range(heads)], axis=1
        )

    num = own_tree[:, :width]
    for i in range(kv_size):
        num = num + spread(scales[i]) * parts[i]
    result = (num / spread(den)).astype(BF16)
    attended[...] = result

    slot = j * per_owner + lax.rem(k, per_owner)
    second = []
    for s in range(kv_size):
        dst = lax.rem(k + s, kv_size)
        second.append(
            pltpu.make_async_remote_copy(
                src_ref=attended, dst_ref=rows_in.at[slot], send_sem=send2.at[s],
                recv_sem=recv2.at[slot], device_id={"kv": dst, "tp": owner},
            )
        )
    for c in second[1:]:
        c.start()

    @pl.when(owner != j)
    def _():
        second[0].start()

    @pl.when(owner == j)
    def _():
        rows_in[slot] = result

    final = final[0:1, :]
    for b in range(seqs):
        at = (2 + b) * heads
        column = jnp.concatenate([final[:, at + h : at + h + 1] for h in range(heads)], axis=0)
        new_gates[b] = jnp.where(chosen[b], placed[b] + column, gates[b])

    for s in range(1, tp_size):
        src = lax.rem(j + tp_size - s, tp_size)
        pltpu.make_async_remote_copy(
            src_ref=weight, dst_ref=weights_in.at[src], send_sem=send3.at[s],
            recv_sem=recv3.at[src], device_id={"tp": src},
        ).wait_recv()
    for i in range(slots):
        from_k = j * per_owner + i % per_owner
        from_j = i // per_owner

        @pl.when(jnp.logical_or(from_k != k, from_j != j))
        def _():
            pltpu.make_async_remote_copy(
                src_ref=attended, dst_ref=rows_in.at[i], send_sem=send2.at[0],
                recv_sem=recv2.at[i], device_id={"kv": from_k, "tp": from_j},
            ).wait_recv()

    out = None
    for g in range(tp_size):
        left = jnp.concatenate(
            [rows_in[g * per_owner + i].astype(F32) for i in range(per_owner)], axis=0
        ).astype(BF16)
        term = jnp.dot(left, weights_in[g], preferred_element_type=F32).astype(BF16).astype(F32)
        out = term if out is None else out + term
    mixed[...] = out.astype(BF16)
    for c in first + third + second[1:]:
        c.wait_send()

    @pl.when(owner != j)
    def _():
        second[0].wait_send()


def body(
    kv_size, tp_size,
    tokens, mix_gain, query_weight, key_weight, value_weight, gate_weight, gate_bias,
    query_gain, key_gain, cache_keys, cache_values, cached_gates, filled, accepted,
    parents, out_weight,
):
    row_count, model = tokens.shape
    seqs, length, width = cache_keys.shape
    heads = cached_gates.shape[1]
    props = parents.shape[1]
    vm = pl.BlockSpec(memory_space=VMEM)
    sm = pl.BlockSpec(memory_space=pltpu.SMEM)
    hbm = pl.BlockSpec(memory_space=pl.ANY)
    wide = width + LANES
    piece = row_count // kv_size
    message, *carried, new_keys, new_values = pl.pallas_call(
        head_kernel,
        out_shape=(
            jax.ShapeDtypeStruct((kv_size, piece, wide), BF16),
            jax.ShapeDtypeStruct((row_count, width), BF16),
            jax.ShapeDtypeStruct((row_count, width), BF16),
            jax.ShapeDtypeStruct((row_count, width), BF16),
            jax.ShapeDtypeStruct((row_count, LANES), F32),
            jax.ShapeDtypeStruct((LANES, row_count), F32),
            jax.ShapeDtypeStruct((row_count, row_count), F32),
            jax.ShapeDtypeStruct(cache_keys.shape, BF16),
            jax.ShapeDtypeStruct(cache_values.shape, BF16),
        ),
        in_specs=[vm] * 8 + [sm] * 2 + [hbm] * 5,
        out_specs=[vm] * 7 + [hbm] * 2,
        scratch_shapes=[
            VMEM((3, model, width), BF16),
            VMEM(cache_keys.shape, BF16),
            VMEM(cache_values.shape, BF16),
            pltpu.SemaphoreType.DMA((3,)),
            pltpu.SemaphoreType.DMA((seqs,)),
            pltpu.SemaphoreType.DMA((seqs,)),
            pltpu.SemaphoreType.DMA((2, seqs)),
        ],
        compiler_params=pltpu.CompilerParams(vmem_limit_bytes=62 * 2**20),
        cost_estimate=pl.CostEstimate(
            flops=500_000_000, bytes_accessed=8 * 2**20, transcendentals=0
        ),
        name="head",
    )(
        tokens, mix_gain.reshape(1, -1), jnp.transpose(gate_weight), gate_bias.reshape(1, -1),
        query_gain.reshape(1, -1), key_gain.reshape(1, -1), cached_gates, parents,
        filled, accepted, query_weight, key_weight, value_weight, cache_keys, cache_values,
    )
    slots = tp_size * (row_count // tp_size // piece)
    dma = pltpu.SemaphoreType.DMA
    mixed, new_gates = pl.pallas_call(
        partial(tail_kernel, kv_size, tp_size, heads),
        out_shape=(
            jax.ShapeDtypeStruct((row_count // tp_size, out_weight.shape[1]), BF16),
            jax.ShapeDtypeStruct(cached_gates.shape, F32),
        ),
        in_specs=[vm] * 9 + [sm] * 2,
        out_specs=[vm] * 2,
        scratch_shapes=[
            VMEM((kv_size, piece, wide), F32),
            VMEM((kv_size, piece, wide), BF16),
            VMEM((piece, width), BF16),
            VMEM((slots, piece, width), BF16),
            VMEM((tp_size,) + out_weight.shape, BF16),
            dma((kv_size,)), dma((kv_size,)), dma((kv_size,)), dma((slots,)),
            dma((tp_size,)), dma((tp_size,)),
        ],
        compiler_params=pltpu.CompilerParams(
            collective_id=0, has_side_effects=True, vmem_limit_bytes=62 * 2**20
        ),
        name="tail",
    )(
        message, *carried, cached_gates, out_weight, filled, accepted,
    )
    return (mixed, new_keys, new_values, new_gates)


def solution(mesh):
    return jax.shard_map(
        partial(body, mesh.shape["kv"], mesh.shape["tp"]),
        mesh=mesh,
        in_specs=(
            P(), P(), P(None, "tp"), P(None, "tp"), P(None, "tp"), P(), P(), P(), P(),
            P(None, "kv", "tp"), P(None, "kv", "tp"), P(None, "tp", "kv"), P(), P(), P(),
            P("tp", "kv"),
        ),
        out_specs=(P("tp", "kv"), P(None, "kv", "tp"), P(None, "kv", "tp"), P(None, "tp", "kv")),
        check_vma=False,
    )
```
